768 devices in a mesh: fs: 96 (over z, y), tp: 8 (over x, core).
Axes of the slice: x: 4, y: 8, z: 12, core: 2. Of those that a mesh axis runs over, the one named last changes fastest.
Arguments:
- tokens: bfloat16 [24576, 1344], P('fs'), may hold values from -6 to 6
- cotangent: bfloat16 [24576, 1344], P('fs'), may hold values from -20 to 20
- gate_weight: bfloat16 [1344, 3072], P('fs', 'tp'), may hold values from -0.15625 to 0.15625
- up_weight: bfloat16 [1344, 3072], P('fs', 'tp'), may hold values from -0.15625 to 0.15625
- down_weight: bfloat16 [3072, 1344], P('tp', 'fs'), may hold values from -0.109375 to 0.109375
Outputs:
- input_grad: bfloat16 [24576, 1344], P('fs')
- down_grad: float32 [3072, 1344], P('tp', 'fs')
The draws below stay inside these ranges and needn't reach their ends.
All inputs are finite; a program needn't handle non-finite values.
Results may differ from the reference program's by a relative error of at most 0.013.
Values may be sent and summed in bfloat16 or wider, within the bound.
No kernel may reach another device: no remote copies, remote signals or barrier semaphores. Data moves between devices by JAX's collectives and lax.ppermute only.
A program may use at most 64 MiB of HBM per device.

```python
import jax
import jax.numpy as jnp
from jax import lax

D = 1344
FF = 3072
TOKENS = 24576
N_TP = 8


def with_spikes(values, key, source, target, blocks, factor):
    owner, partner = [(jnp.arange(values.shape[position]) // (values.shape[position] // blocks)).reshape([-1 if axis == position else 1 for axis in range(values.ndim)]) for position in (source, target)]
    chosen = jax.random.permutation(key, blocks)[partner]
    strong = (owner == chosen) | (owner == (partner + blocks // 2) % blocks)
    return jnp.where(strong, factor * values, values)


def steps_of(stream_key, dims, split, least, largest):
    factor_of, own = 1.0, jax.random.fold_in(stream_key, 6)
    for axis_at, blocks in split:
        heights = jnp.exp(jax.random.uniform(jax.random.fold_in(own, axis_at), (blocks,), jnp.float32, least / len(split), largest / len(split)))
        factor_of = factor_of * jnp.repeat(heights, dims[axis_at] // blocks).reshape([-1 if axis == axis_at else 1 for axis in range(len(dims))])
    return factor_of


def scatter_about(rng, shape, width, limit, split=(), held_as=jnp.bfloat16):
    level = steps_of(rng, shape, split, -0.22, 0.18) if split else 1.0
    values = jax.random.normal(rng, shape, jnp.float32) * width * level
    return jnp.minimum(jnp.maximum(values, -limit), limit).astype(held_as)


def bell_draw_with(key, extent, spread, limit, shards, heavy, dtype=jnp.bfloat16):
    result = spread * jax.random.normal(key, extent, jnp.float32)
    if shards:
        result = result * steps_of(key, extent, shards, -0.22, 0.18)
    return jnp.clip(with_spikes(result, jax.random.fold_in(key, 3), *heavy), -limit, limit).astype(dtype)


def setup_inputs(seed: int = 0) -> dict:
    streams_of = jax.random.split(jax.random.key(seed), 6)
    tokens = scatter_about(streams_of[0], (TOKENS, D), 1.0, 6.0, ((0, 96),))
    cotangent = bell_draw_with(streams_of[1], (TOKENS, D), 1.0, 20.0, ((0, 96),), (0, 1, 96, 4.75))
    gate_weight = scatter_about(streams_of[2], (D, FF), D ** -0.5, 0.15625, ((0, 96), (1, 8)))
    up_weight = scatter_about(streams_of[3], (D, FF), D ** -0.5, 0.15625, ((0, 96), (1, 8)))
    down_weight = scatter_about(streams_of[4], (FF, D), FF ** -0.5, 0.109375, ((0, 8), (1, 96)))
    return dict(tokens=tokens, cotangent=cotangent, gate_weight=gate_weight, up_weight=up_weight, down_weight=down_weight)


def contract_rows(left, right):
    return lax.dot_general(left, right, (((0,), (0,)), ((), ())), preferred_element_type=jnp.float32)


def contract_cols(left, right):
    return lax.dot_general(left, right, (((1,), (1,)), ((), ())), preferred_element_type=jnp.float32)


def reference(tokens, cotangent, gate_weight, up_weight, down_weight):
    gate_pre = jnp.dot(tokens, gate_weight, preferred_element_type=jnp.float32)
    up_pre = jnp.dot(tokens, up_weight, preferred_element_type=jnp.float32)
    sigmoid_gate = jax.nn.sigmoid(gate_pre)
    activated = gate_pre * sigmoid_gate
    hidden = (activated * up_pre).astype(jnp.bfloat16)
    hidden_grad = contract_cols(cotangent, down_weight)
    gate_pre_grad = (hidden_grad * up_pre * sigmoid_gate * (1.0 + gate_pre * (1.0 - sigmoid_gate))).astype(jnp.bfloat16)
    up_pre_grad = (hidden_grad * activated).astype(jnp.bfloat16)
    block_width = FF // N_TP
    summed = jnp.zeros(tokens.shape, jnp.float32)
    for member in range(N_TP):
        lower = member * block_width
        upper = lower + block_width
        partial_value = contract_cols(gate_pre_grad[:, lower:upper], gate_weight[:, lower:upper])
        partial_value = partial_value + contract_cols(up_pre_grad[:, lower:upper], up_weight[:, lower:upper])
        summed = summed + partial_value.astype(jnp.bfloat16).astype(jnp.float32)
    input_grad = summed.astype(jnp.bfloat16)
    down_grad = contract_rows(hidden, cotangent)
    return input_grad, down_grad
```

```python
import jax
import jax.numpy as jnp
import numpy as np
from jax import lax
from jax.sharding import Mesh
from jax.sharding import PartitionSpec as P

FS = ("fs_0", "fs_1")


def shifted(array, axis, step):
    peers = lax.axis_size(axis)
    return lax.ppermute(array, axis, [(k, (k + step) % peers) for k in range(peers)])


def sent_to_all(array, axis):
    peers = lax.axis_size(axis)
    return lax.all_to_all(
        jnp.broadcast_to(array[None], (peers, *array.shape)), axis, 0, 0, tiled=True
    )


def exchanged(parts, axis):
    got = lax.all_to_all(parts, axis, 0, 0, tiled=True)
    return got.astype(jnp.float32).sum(axis=0)


def contract_rows(left, right):
    return lax.dot_general(
        left, right, (((0,), (0,)), ((), ())), preferred_element_type=jnp.float32
    )


def contract_cols(left, right):
    return lax.dot_general(
        left, right, (((1,), (1,)), ((), ())), preferred_element_type=jnp.float32
    )


def inner_first(width, outer, inner):
    rows = width // (outer * inner)
    return np.arange(width).reshape(outer, inner, rows).transpose(1, 0, 2).reshape(-1)


def ring_order(width, offsets):
    blocks = np.arange(width).reshape(len(offsets), -1)
    return np.concatenate([blocks[k] for k in offsets])


def picked(source):
    source = jnp.asarray(source, jnp.int32)
    spot = lax.broadcasted_iota(jnp.int32, (source.size, source.size), 1)
    return (source[:, None] == spot).astype(jnp.bfloat16)


def gathered(block, axis, stride):
    peers = lax.axis_size(axis)
    steps = range(stride, peers, stride)
    held = jnp.concatenate([block] + [shifted(block, axis, s) for s in steps])
    offsets = [-s % peers for s in range(0, peers, stride)]
    whole, order = [held], list(offsets)
    for step in (1, -1):
        whole.append(shifted(held, axis, step))
        order += [(k - step) % peers for k in offsets]
    return jnp.concatenate(whole), order


def summed_over_tp(partial):
    half = partial.shape[0] // 2
    core = lax.axis_index("core")
    kept = lax.dynamic_slice_in_dim(partial, core * half, half)
    given = lax.dynamic_slice_in_dim(partial, (1 - core) * half, half)
    kept = kept.astype(jnp.float32) + shifted(given, "core", 1).astype(jnp.float32)
    kept = kept.astype(jnp.bfloat16)
    chips = lax.axis_size("chip")
    others = [shifted(kept, "chip", s) for s in range(1, chips)]
    total = kept.astype(jnp.float32)
    for other in others:
        total = total + other.astype(jnp.float32)
    total = total.astype(jnp.bfloat16)
    other = shifted(total, "core", 1)
    first = jnp.where(core == 0, total, other)
    second = jnp.where(core == 0, other, total)
    return jnp.concatenate([first, second])


def per_device(tokens, cotangent, gate_weight, up_weight, down_weight):
    outer, inner = (lax.axis_size(a) for a in FS)
    rows, units = gate_weight.shape
    width = tokens.shape[1]
    place = lax.axis_index("fs_0")

    gate_up = jnp.concatenate([gate_weight, up_weight], axis=1)
    gate_up = sent_to_all(gate_up, "fs_1").reshape(inner * rows, 2 * units)
    down = sent_to_all(down_weight.T, "fs_0").reshape(outer * rows, units)
    down = sent_to_all(down, "fs_1").reshape(width, units)
    gate_up, order = gathered(gate_up, "fs_0", 3)

    here = picked((ring_order(width, order) + place * (inner * rows)) % width)
    turned_tokens = contract_cols(here, tokens).astype(jnp.bfloat16)
    turned_cotangent = contract_cols(picked(inner_first(width, outer, inner)), cotangent).astype(
        jnp.bfloat16
    )

    both = contract_rows(turned_tokens, gate_up)
    gate_pre, up_pre = both[:, :units], both[:, units:]
    sigmoid_gate = jax.nn.sigmoid(gate_pre)
    activated = gate_pre * sigmoid_gate
    hidden = (activated * up_pre).astype(jnp.bfloat16)

    terms = jnp.dot(turned_cotangent, hidden, preferred_element_type=jnp.float32)
    terms = terms.astype(jnp.bfloat16).reshape(inner, outer * rows, units)
    terms = exchanged(terms, "fs_1").astype(jnp.bfloat16)
    down_grad = exchanged(terms.reshape(outer, rows, units), "fs_0").T

    hidden_grad = contract_rows(turned_cotangent, down)
    gate_pre_grad = (
        hidden_grad * up_pre * sigmoid_gate * (1.0 + gate_pre * (1.0 - sigmoid_gate))
    ).astype(jnp.bfloat16)
    up_pre_grad = (hidden_grad * activated).astype(jnp.bfloat16)
    partial = contract_cols(gate_up, jnp.concatenate([gate_pre_grad, up_pre_grad], axis=1))
    total = summed_over_tp(partial.astype(jnp.bfloat16))
    input_grad = contract_rows(total, here).astype(jnp.bfloat16)
    return (input_grad, down_grad)


def solution(mesh):
    torus = Mesh(
        mesh.devices.reshape(12, 8, mesh.shape["tp"] // 2, 2), ("fs_0", "fs_1", "chip", "core")
    )
    tp = ("chip", "core")
    in_specs = (P(FS, None), P(FS, None), P(FS, tp), P(FS, tp), P(tp, FS))
    out_specs = (P(FS, None), P(tp, FS))
    return jax.shard_map(
        per_device, mesh=torus, in_specs=in_specs, out_specs=out_specs, check_vma=False
    )
```

```python
import jax
import jax.numpy as jnp
import numpy as np
from jax import lax
from jax.sharding import Mesh
from jax.sharding import PartitionSpec as P


FS = ("fs_0", "fs_1")


def shifted(array, axis, step):
    peers = lax.axis_size(axis)
    return lax.ppermute(array, axis, [(k, (k + step) % peers) for k in range(peers)])


def sent_to_all(array, axis):
    peers = lax.axis_size(axis)
    return lax.all_to_all(
        jnp.broadcast_to(array[None], (peers, *array.shape)), axis, 0, 0, tiled=True
    )


def exchanged(parts, axis):
    got = lax.all_to_all(parts, axis, 0, 0, tiled=True)
    return got.astype(jnp.float32).sum(axis=0)


def contract_rows(left, right):
    return lax.dot_general(
        left, right, (((0,), (0,)), ((), ())), preferred_element_type=jnp.float32
    )


def contract_cols(left, right):
    return lax.dot_general(
        left, right, (((1,), (1,)), ((), ())), preferred_element_type=jnp.float32
    )


def inner_first(width, outer, inner):
    rows = width // (outer * inner)
    return np.arange(width).reshape(outer, inner, rows).transpose(1, 0, 2).reshape(-1)


def picked(source):
    source = jnp.asarray(source, jnp.int32)
    spot = lax.broadcasted_iota(jnp.int32, (source.size, source.size), 1)
    return (source[:, None] == spot).astype(jnp.bfloat16)


def around(blocks, axis):
    peers = lax.axis_size(axis)
    split = blocks[0].shape[0] // 16 * 8
    ups = downs = blocks
    parts, order = [[b] for b in blocks], [0]
    for step in range(1, peers // 2):
        moved = [(shifted(u, axis, 1), shifted(d, axis, -1)) for u, d in zip(ups, downs)]
        ups, downs = zip(*moved)
        for held, pair in zip(parts, moved):
            held += pair
        order += [-step % peers, step]
    for held, u, d in zip(parts, ups, downs):
        held += [shifted(u[:split], axis, 1), shifted(d[split:], axis, -1)]
    return [jnp.concatenate(held) for held in parts], order + [peers // 2]


def summed_over_tp(partial, after):
    half = partial.shape[0] // 2
    core = lax.axis_index("core")
    kept = lax.dynamic_slice_in_dim(partial, core * half, half)
    given = lax.dynamic_slice_in_dim(partial, (1 - core) * half, half)
    kept = kept.astype(jnp.float32) + shifted(given, "core", 1).astype(jnp.float32)
    kept = kept.astype(jnp.bfloat16)
    chips = lax.axis_size("chip")
    others = [shifted(kept, "chip", s) for s in range(1, chips)]
    *others, _ = lax.optimization_barrier((*others, after))
    total = kept.astype(jnp.float32)
    for other in others:
        total = total + other.astype(jnp.float32)
    total = total.astype(jnp.bfloat16)
    other = shifted(total, "core", 1)
    first = jnp.where(core == 0, total, other)
    second = jnp.where(core == 0, other, total)
    return jnp.concatenate([first, second])


def gradients(tokens, cotangent, gate_weight, up_weight, down_weight):
    outer, inner = (lax.axis_size(a) for a in FS)
    rows, units = gate_weight.shape
    width = tokens.shape[1]
    place = lax.axis_index("fs_1")

    weights = jnp.concatenate([gate_weight, up_weight, down_weight.T], axis=1)
    weights = sent_to_all(weights, "fs_0").reshape(outer * rows, 3 * units)
    (gate_up, down), order = around((weights[:, : 2 * units], weights[:, 2 * units :]), "fs_1")

    spot = inner_first(width, outer, inner)
    block = (jnp.asarray(order, jnp.int32) + place) % inner
    near = (block[:, None] * rows + spot[: outer * rows][None, :]).reshape(-1)
    here = picked(near)
    near_tokens = contract_cols(here, tokens).astype(jnp.bfloat16)
    near_cotangent = contract_cols(here, cotangent).astype(jnp.bfloat16)
    turned_cotangent = contract_cols(picked(spot), cotangent).astype(jnp.bfloat16)
    near_tokens, near_cotangent, turned_cotangent = lax.optimization_barrier(
        (near_tokens, near_cotangent, turned_cotangent)
    )

    both = contract_rows(near_tokens, gate_up)
    gate_pre, up_pre = both[:, :units], both[:, units:]
    sigmoid_gate = jax.nn.sigmoid(gate_pre)
    activated = gate_pre * sigmoid_gate
    hidden = (activated * up_pre).astype(jnp.bfloat16)

    terms = jnp.dot(turned_cotangent, hidden, preferred_element_type=jnp.float32)
    terms = terms.astype(jnp.bfloat16).reshape(inner, outer * rows, units)
    terms = exchanged(terms, "fs_1").astype(jnp.bfloat16).reshape(outer, rows, units)

    hidden_grad = contract_rows(near_cotangent, down)
    gate_pre_grad = (
        hidden_grad * up_pre * sigmoid_gate * (1.0 + gate_pre * (1.0 - sigmoid_gate))
    ).astype(jnp.bfloat16)
    up_pre_grad = (hidden_grad * activated).astype(jnp.bfloat16)
    partial = contract_cols(gate_up, jnp.concatenate([gate_pre_grad, up_pre_grad], axis=1))
    total = summed_over_tp(partial.astype(jnp.bfloat16), terms)
    down_grad = exchanged(terms, "fs_0").T
    input_grad = contract_rows(total, here).astype(jnp.bfloat16)
    return (input_grad, down_grad)


def solution(mesh):
    torus = Mesh(
        mesh.devices.reshape(12, 8, mesh.shape["tp"] // 2, 2), ("fs_0", "fs_1", "chip", "core")
    )
    tp = ("chip", "core")
    in_specs = (P(FS, None), P(FS, None), P(FS, tp), P(FS, tp), P(tp, FS))
    out_specs = (P(FS, None), P(tp, FS))
    return jax.shard_map(
        gradients, mesh=torus, in_specs=in_specs, out_specs=out_specs, check_vma=False
    )
```

```python
import jax
import jax.numpy as jnp
import numpy as np
from jax import lax
from jax.sharding import Mesh
from jax.sharding import PartitionSpec as P


FS = ("fs_0", "fs_1")


def shifted(array, axis, step):
    peers = lax.axis_size(axis)
    return lax.ppermute(array, axis, [(k, (k + step) % peers) for k in range(peers)])


def sent_to_all(array, axis):
    peers = lax.axis_size(axis)
    return lax.all_to_all(
        jnp.broadcast_to(array[None], (peers, *array.shape)), axis, 0, 0, tiled=True
    )


def exchanged(parts, axis):
    got = lax.all_to_all(parts, axis, 0, 0, tiled=True)
    return got.astype(jnp.float32).sum(axis=0)


def contract_rows(left, right):
    return lax.dot_general(
        left, right, (((0,), (0,)), ((), ())), preferred_element_type=jnp.float32
    )


def contract_cols(left, right):
    return lax.dot_general(
        left, right, (((1,), (1,)), ((), ())), preferred_element_type=jnp.float32
    )


def inner_first(width, outer, inner):
    rows = width // (outer * inner)
    return np.arange(width).reshape(outer, inner, rows).transpose(1, 0, 2).reshape(-1)


def picked(source):
    source = jnp.asarray(source, jnp.int32)
    spot = lax.broadcasted_iota(jnp.int32, (source.size, source.size), 1)
    return (source[:, None] == spot).astype(jnp.bfloat16)


def swung(array, axis, step):
    peers = lax.axis_size(axis)
    ways = [(core, step if core == 0 else -step) for core in range(2)]
    pairs = [
        (2 * k + core, 2 * ((k + way) % peers) + core) for k in range(peers) for core, way in ways
    ]
    return lax.ppermute(array, (axis, "core"), pairs)


def around(block, axis, widths):
    peers = lax.axis_size(axis)
    rows = block.shape[0]
    split = rows // 16 * 8
    place = lax.axis_index(axis)
    way = 1 - 2 * lax.axis_index("core")
    ends = np.cumsum(widths)
    wholes = [jnp.zeros((peers, rows, w), block.dtype) for w in widths]

    def put(part, owner, start):
        owner = (owner + peers) % peers
        for k, (end, w) in enumerate(zip(ends, widths)):
            piece = part[None, :, end - w : end]
            wholes[k] = lax.dynamic_update_slice(wholes[k], piece, (owner, start, 0))

    put(block, place, 0)
    up = down = block
    for step in range(1, peers // 2):
        up, down = swung(up, axis, 1), swung(down, axis, -1)
        put(up, place - step * way, 0)
        put(down, place + step * way, 0)
    put(swung(up[:split], axis, 1), place + peers // 2, 0)
    put(swung(down[split:], axis, -1), place + peers // 2, split)
    return [w.reshape(peers * rows, -1) for w in wholes]


def summed_over_tp(partial, after):
    half = partial.shape[0] // 2
    core = lax.axis_index("core")
    kept = lax.dynamic_slice_in_dim(partial, core * half, half)
    given = lax.dynamic_slice_in_dim(partial, (1 - core) * half, half)
    kept = kept.astype(jnp.float32) + shifted(given, "core", 1).astype(jnp.float32)
    kept = kept.astype(jnp.bfloat16)
    chips = lax.axis_size("chip")
    others = [shifted(kept, "chip", s) for s in range(1, chips)]
    *others, _ = lax.optimization_barrier((*others, after))
    total = kept.astype(jnp.float32)
    for other in others:
        total = total + other.astype(jnp.float32)
    total = total.astype(jnp.bfloat16)
    other = shifted(total, "core", 1)
    first = jnp.where(core == 0, total, other)
    second = jnp.where(core == 0, other, total)
    return jnp.concatenate([first, second])


def gradients(tokens, cotangent, gate_weight, up_weight, down_weight):
    outer, inner = (lax.axis_size(a) for a in FS)
    rows, units = gate_weight.shape
    width = tokens.shape[1]
    weights = jnp.concatenate([gate_weight, up_weight, down_weight.T], axis=1)
    weights = sent_to_all(weights, "fs_0").reshape(outer * rows, 3 * units)
    gate_up, down = around(weights, "fs_1", (2 * units, units))

    turn = lax.optimization_barrier(picked(inner_first(width, outer, inner)))
    turned_tokens = contract_cols(turn, tokens).astype(jnp.bfloat16)
    turned_cotangent = contract_cols(turn, cotangent).astype(jnp.bfloat16)
    turned_tokens, turned_cotangent = lax.optimization_barrier((turned_tokens, turned_cotangent))

    both = contract_rows(turned_tokens, gate_up)
    gate_pre, up_pre = both[:, :units], both[:, units:]
    sigmoid_gate = jax.nn.sigmoid(gate_pre)
    activated = gate_pre * sigmoid_gate
    hidden = (activated * up_pre).astype(jnp.bfloat16)

    terms = jnp.dot(turned_cotangent, hidden, preferred_element_type=jnp.float32)
    terms = terms.astype(jnp.bfloat16).reshape(inner, outer * rows, units)
    terms = exchanged(terms, "fs_1").astype(jnp.bfloat16).reshape(outer, rows, units)

    hidden_grad = contract_rows(turned_cotangent, down)
    gate_pre_grad = (
        hidden_grad * up_pre * sigmoid_gate * (1.0 + gate_pre * (1.0 - sigmoid_gate))
    ).astype(jnp.bfloat16)
    up_pre_grad = (hidden_grad * activated).astype(jnp.bfloat16)
    partial = contract_cols(gate_up, jnp.concatenate([gate_pre_grad, up_pre_grad], axis=1))
    total = summed_over_tp(partial.astype(jnp.bfloat16), terms)
    down_grad = exchanged(terms, "fs_0").T
    input_grad = contract_rows(total, turn).astype(jnp.bfloat16)
    return (input_grad, down_grad)


def solution(mesh):
    torus = Mesh(
        mesh.devices.reshape(12, 8, mesh.shape["tp"] // 2, 2), ("fs_0", "fs_1", "chip", "core")
    )
    tp = ("chip", "core")
    in_specs = (P(FS, None), P(FS, None), P(FS, tp), P(FS, tp), P(tp, FS))
    out_specs = (P(FS, None), P(tp, FS))
    return jax.shard_map(
        gradients, mesh=torus, in_specs=in_specs, out_specs=out_specs, check_vma=False
    )
```

```python
import jax
import jax.numpy as jnp
import numpy as np
from jax import lax
from jax.sharding import Mesh
from jax.sharding import PartitionSpec as P


FAR = 4
CHAINS = 2
FS_0 = ("fs_0h", "fs_0l")
FS = (*FS_0, "fs_1")


def shifted(array, axis, step):
    peers = lax.axis_size(axis)
    return lax.ppermute(array, axis, [(k, (k + step) % peers) for k in range(peers)])


def paired(array, axis, turn):
    peers = lax.axis_size(axis)
    pairs = []
    for k in range(peers):
        for core in range(2):
            other = (k + (1 if (k + core + turn) % 2 == 0 else -1)) % peers
            pairs.append((2 * k + core, 2 * other + core))
    return lax.ppermute(array, (*axis, "core"), pairs)


def sent_to_all(array, axis):
    peers = lax.axis_size(axis)
    return lax.all_to_all(
        jnp.broadcast_to(array[None], (peers, *array.shape)), axis, 0, 0, tiled=True
    )


def exchanged(parts, axis):
    got = lax.all_to_all(parts, axis, 0, 0, tiled=True)
    return got.astype(jnp.float32).sum(axis=0)


def contract_cols(left, right):
    return lax.dot_general(
        left, right, (((1,), (1,)), ((), ())), preferred_element_type=jnp.float32
    )


def picked(source):
    source = jnp.asarray(source, jnp.int32)
    spot = lax.broadcasted_iota(jnp.int32, (source.size, source.size), 1)
    return (source[:, None] == spot).astype(jnp.bfloat16)


def around(block, axis):
    peers = lax.axis_size(axis)
    rows = block.shape[0] // CHAINS
    place = lax.axis_index(axis)
    role = (place + lax.axis_index("core")) % 2
    whole = jnp.zeros((peers, *block.shape), block.dtype)

    def put(whole, part, owner, chain):
        owner = (owner + 2 * peers) % peers
        return lax.dynamic_update_slice(whole, part[None], (owner, chain * rows, 0))

    base = place - role
    own = [block[k * rows : (k + 1) * rows] for k in range(CHAINS)]
    got = [paired(b, axis, 0) for b in own]
    for k in range(CHAINS):
        whole = put(whole, own[k], place, k)
        whole = put(whole, got[k], base + 1 - role, k)
    held = [jnp.stack(pair) for pair in zip(own, got)]
    for step in range(1, peers // 2):
        held = [paired(h, axis, step) for h in held]
        odd = step % 2
        away = (step + 1) // 2 * (1 - 2 * odd) * (1 - 2 * role)
        first = odd + role - 2 * odd * role
        for k, h in enumerate(held):
            whole = put(whole, h[0], base + 2 * away + first, k)
            whole = put(whole, h[1], base + 2 * away + 1 - first, k)
    return whole.reshape(peers * block.shape[0], -1)


def added(left, right):
    return (left.astype(jnp.float32) + right.astype(jnp.float32)).astype(jnp.bfloat16)


def summed_over_tp(partial):
    half = partial.shape[0] // 2
    core = lax.axis_index("core")
    kept = lax.dynamic_slice_in_dim(partial, core * half, half)
    given = lax.dynamic_slice_in_dim(partial, (1 - core) * half, half)
    total = added(kept, shifted(given, "core", 1))
    total = added(total, paired(total, ("chip",), 0))
    other = paired(total, ("chip",), 1)
    total = added(total, other)
    other = shifted(total, "core", 1)
    first = jnp.where(core == 0, total, other)
    second = jnp.where(core == 0, other, total)
    return jnp.concatenate([first, second])


def gradients(tokens, cotangent, gate_weight, up_weight, down_weight):
    near, inner = lax.axis_size("fs_0l"), lax.axis_size("fs_1")
    rows, units = gate_weight.shape
    width = tokens.shape[1]

    weights = jnp.concatenate([gate_weight, up_weight, down_weight.T], axis=1)
    weights = sent_to_all(weights, "fs_1").reshape(inner * rows, 3 * units)
    weights = around(weights, FS_0)
    gate_up, down = weights[:, : 2 * units], weights[:, 2 * units :]

    spot = np.arange(width).reshape(FAR, near, inner, rows).transpose(2, 1, 0, 3).reshape(-1)
    turned_cotangent = contract_cols(picked(spot), cotangent).astype(jnp.bfloat16)
    turned_cotangent = lax.optimization_barrier(turned_cotangent)

    both = jnp.dot(tokens, gate_up, preferred_element_type=jnp.float32)
    gate_pre, up_pre = both[:, :units], both[:, units:]
    sigmoid_gate = jax.nn.sigmoid(gate_pre)
    activated = gate_pre * sigmoid_gate
    hidden = (activated * up_pre).astype(jnp.bfloat16)

    terms = jnp.dot(turned_cotangent, hidden, preferred_element_type=jnp.float32)
    terms = terms.astype(jnp.bfloat16).reshape(inner * near, FAR * rows, units)
    terms = exchanged(terms, ("fs_1", "fs_0l"))
    terms = terms.astype(jnp.bfloat16).reshape(FAR, rows, units)
    down_grad = exchanged(terms, "fs_0h").T

    hidden_grad = jnp.dot(cotangent, down, preferred_element_type=jnp.float32)
    gate_pre_grad = (
        hidden_grad * up_pre * sigmoid_gate * (1.0 + gate_pre * (1.0 - sigmoid_gate))
    ).astype(jnp.bfloat16)
    up_pre_grad = (hidden_grad * activated).astype(jnp.bfloat16)
    partial = contract_cols(gate_up, jnp.concatenate([gate_pre_grad, up_pre_grad], axis=1))
    total = summed_over_tp(partial.astype(jnp.bfloat16))
    return (total.T, down_grad)


def solution(mesh):
    torus = Mesh(
        mesh.devices.reshape(FAR, 12 // FAR, 8, mesh.shape["tp"] // 2, 2), (*FS, "chip", "core")
    )
    tp = ("chip", "core")
    in_specs = (P(FS, None), P(FS, None), P(FS, tp), P(FS, tp), P(tp, FS))
    out_specs = (P(FS, None), P(tp, FS))
    return jax.shard_map(
        gradients, mesh=torus, in_specs=in_specs, out_specs=out_specs, check_vma=False
    )
```

```python
import jax
import jax.numpy as jnp
import numpy as np
from jax import lax
from jax.sharding import Mesh
from jax.sharding import PartitionSpec as P


FAR = 4
FS_0 = ("fs_0h", "fs_0l")
FS_1 = ("fs_1h", "fs_1l")
FS = (*FS_0, *FS_1)


def shifted(array, axis, step):
    peers = lax.axis_size(axis)
    return lax.ppermute(array, axis, [(k, (k + step) % peers) for k in range(peers)])


def sent_to_all(array, axis):
    peers = lax.axis_size(axis)
    return lax.all_to_all(
        jnp.broadcast_to(array[None], (peers, *array.shape)), axis, 0, 0, tiled=True
    )


def exchanged(parts, axis):
    got = lax.all_to_all(parts, axis, 0, 0, tiled=True)
    return got.astype(jnp.float32).sum(axis=0)


def contract_rows(left, right):
    return lax.dot_general(
        left, right, (((0,), (0,)), ((), ())), preferred_element_type=jnp.float32
    )


def contract_cols(left, right):
    return lax.dot_general(
        left, right, (((1,), (1,)), ((), ())), preferred_element_type=jnp.float32
    )


def picked(source):
    source = jnp.asarray(source, jnp.int32)
    spot = lax.broadcasted_iota(jnp.int32, (source.size, source.size), 1)
    return (source[:, None] == spot).astype(jnp.bfloat16)


def gathered(block):
    block = sent_to_all(block, (FS_0[0], FS_1[0]))
    block = block.reshape(-1, block.shape[2])
    rows, columns = block.shape
    near = lax.axis_size(FS_0[1])
    place = lax.axis_index(FS_0[1])
    held = jnp.zeros((near, rows, columns), block.dtype)
    for part, owner in (
        (block, place),
        (shifted(block, FS_0, 1), (place + near - 1) % near),
        (shifted(block, FS_0, -1), (place + 1) % near),
    ):
        held = lax.dynamic_update_slice(held, part[None], (owner, 0, 0))
    held = held.reshape(near * rows, columns)
    half = near * rows // 2
    side = lax.axis_index(FS_1[1])
    whole = jnp.zeros((2, near * rows, columns), block.dtype)
    for part, owner, start in (
        (held, side, 0),
        (shifted(held[:half], FS_1, -1), 1 - side, 0),
        (shifted(held[half:], FS_1, 1), 1 - side, half),
    ):
        whole = lax.dynamic_update_slice(whole, part[None], (owner, start, 0))
    return whole.reshape(2 * near * rows, columns)


def paired(array, turn):
    chips = lax.axis_size("chip")
    pairs = []
    for chip in range(chips):
        for core in range(2):
            other = (chip + (1 if (chip + core + turn) % 2 == 0 else -1)) % chips
            pairs.append((2 * chip + core, 2 * other + core))
    return lax.ppermute(array, ("chip", "core"), pairs)


def added(left, right):
    return (left.astype(jnp.float32) + right.astype(jnp.float32)).astype(jnp.bfloat16)


def summed_over_tp(partial):
    half = partial.shape[0] // 2
    core = lax.axis_index("core")
    kept = lax.dynamic_slice_in_dim(partial, core * half, half)
    given = lax.dynamic_slice_in_dim(partial, (1 - core) * half, half)
    total = added(kept, shifted(given, "core", 1))
    total = added(total, paired(total, 0))
    other = paired(total, 1)
    total = added(total, other)
    other = shifted(total, "core", 1)
    first = jnp.where(core == 0, total, other)
    second = jnp.where(core == 0, other, total)
    return jnp.concatenate([first, second])


def gradients(tokens, cotangent, gate_weight, up_weight, down_weight):
    near, inner = lax.axis_size("fs_0l"), lax.axis_size(FS_1)
    rows, units = gate_weight.shape
    width = tokens.shape[1]

    weights = gathered(jnp.concatenate([gate_weight, up_weight, down_weight.T], axis=1))
    gate_up, down = weights[:, : 2 * units], weights[:, 2 * units :]

    spot = np.arange(width).reshape(FAR, near, inner // 2, 2, rows)
    held = spot.transpose(3, 1, 0, 2, 4).reshape(-1)
    sent = spot.transpose(2, 3, 1, 0, 4).reshape(-1)
    into, back = picked(held), picked(np.argsort(held))
    into, back = lax.optimization_barrier((into, back))
    held_tokens = contract_cols(into, tokens).astype(jnp.bfloat16)
    held_cotangent = contract_cols(into, cotangent).astype(jnp.bfloat16)
    sent_cotangent = contract_cols(picked(sent), cotangent).astype(jnp.bfloat16)
    held_tokens, held_cotangent, sent_cotangent = lax.optimization_barrier(
        (held_tokens, held_cotangent, sent_cotangent)
    )

    both = contract_rows(held_tokens, gate_up)
    gate_pre, up_pre = both[:, :units], both[:, units:]
    sigmoid_gate = jax.nn.sigmoid(gate_pre)
    activated = gate_pre * sigmoid_gate
    hidden = (activated * up_pre).astype(jnp.bfloat16)

    terms = jnp.dot(sent_cotangent, hidden, preferred_element_type=jnp.float32)
    terms = terms.astype(jnp.bfloat16).reshape(inner * near, FAR * rows, units)
    terms = exchanged(terms, (*FS_1, "fs_0l"))
    terms = terms.astype(jnp.bfloat16).reshape(FAR, rows, units)
    down_grad = exchanged(terms, "fs_0h").T

    hidden_grad = contract_rows(held_cotangent, down)
    gate_pre_grad = (
        hidden_grad * up_pre * sigmoid_gate * (1.0 + gate_pre * (1.0 - sigmoid_gate))
    ).astype(jnp.bfloat16)
    up_pre_grad = (hidden_grad * activated).astype(jnp.bfloat16)
    partial = contract_cols(gate_up, jnp.concatenate([gate_pre_grad, up_pre_grad], axis=1))
    partial = jnp.dot(back, partial.astype(jnp.bfloat16), preferred_element_type=jnp.float32)
    total = summed_over_tp(partial.astype(jnp.bfloat16))
    return (total.T, down_grad)


def solution(mesh):
    torus = Mesh(
        mesh.devices.reshape(FAR, 12 // FAR, 4, 2, mesh.shape["tp"] // 2, 2), (*FS, "chip", "core")
    )
    tp = ("chip", "core")
    in_specs = (P(FS, None), P(FS, None), P(FS, tp), P(FS, tp), P(tp, FS))
    out_specs = (P(FS, None), P(tp, FS))
    return jax.shard_map(
        gradients, mesh=torus, in_specs=in_specs, out_specs=out_specs, check_vma=False
    )
```

```python
import jax
import jax.numpy as jnp
from jax import lax
from jax.sharding import Mesh
from jax.sharding import PartitionSpec as P


FAR = 4
FS_0 = ("fs_0h", "fs_0l")
FS = (*FS_0, "fs_1")
WIDE = ("fs_0h", "fs_1")


def shifted(array, axis, step):
    peers = lax.axis_size(axis)
    return lax.ppermute(array, axis, [(k, (k + step) % peers) for k in range(peers)])


def sent_to_all(array, axis):
    peers = lax.axis_size(axis)
    return lax.all_to_all(
        jnp.broadcast_to(array[None], (peers, *array.shape)), axis, 0, 0, tiled=True
    )


def exchanged(parts, axis):
    got = lax.all_to_all(parts, axis, 0, 0, tiled=True)
    return got.astype(jnp.float32).sum(axis=0)


def contract_rows(left, right):
    return lax.dot_general(
        left, right, (((0,), (0,)), ((), ())), preferred_element_type=jnp.float32
    )


def contract_cols(left, right):
    return lax.dot_general(
        left, right, (((1,), (1,)), ((), ())), preferred_element_type=jnp.float32
    )


def next_near(step):
    near = lax.axis_size(FS_0[1])
    return (lax.axis_index(FS_0[1]) + near + step) % near


def gathered(block):
    block = sent_to_all(block, WIDE)
    block = block.reshape(FAR, -1, block.shape[2])
    below, above = shifted(block, FS_0, 1), shifted(block, FS_0, -1)
    shape = (FAR, lax.axis_size(FS_0[1]), *block.shape[1:])
    whole = jnp.zeros(shape, block.dtype)
    for part, step in ((block, 0), (below, -1), (above, 1)):
        whole = lax.dynamic_update_slice(whole, part[:, None], (0, next_near(step), 0, 0))
    return whole.reshape(-1, block.shape[2])


def scattered(terms, rows):
    terms = terms.reshape(FAR, lax.axis_size(FS_0[1]), -1, terms.shape[1])
    mine, over, under = (
        lax.dynamic_index_in_dim(terms, next_near(step), 1, keepdims=False)
        for step in (0, 1, -1)
    )
    total = mine.astype(jnp.float32)
    total = total + shifted(over, FS_0, 1).astype(jnp.float32)
    total = total + shifted(under, FS_0, -1).astype(jnp.float32)
    total = total.astype(jnp.bfloat16).reshape(-1, rows, terms.shape[3])
    return exchanged(total, WIDE)


def paired(array, turn):
    chips = lax.axis_size("chip")
    pairs = []
    for chip in range(chips):
        for core in range(2):
            other = (chip + (1 if (chip + core + turn) % 2 == 0 else -1)) % chips
            pairs.append((2 * chip + core, 2 * other + core))
    return lax.ppermute(array, ("chip", "core"), pairs)


def added(left, right):
    return (left.astype(jnp.float32) + right.astype(jnp.float32)).astype(jnp.bfloat16)


def summed_over_tp(partial):
    half = partial.shape[0] // 2
    core = lax.axis_index("core")
    kept = lax.dynamic_slice_in_dim(partial, core * half, half)
    given = lax.dynamic_slice_in_dim(partial, (1 - core) * half, half)
    total = added(kept, shifted(given, "core", 1))
    total = added(total, paired(total, 0))
    other = paired(total, 1)
    total = added(total, other)
    other = shifted(total, "core", 1)
    first = jnp.where(core == 0, total, other)
    second = jnp.where(core == 0, other, total)
    return jnp.concatenate([first, second])


def gradients(tokens, cotangent, gate_weight, up_weight, down_weight):
    rows, units = gate_weight.shape
    gate_up = gathered(jnp.concatenate([gate_weight, up_weight], axis=1))
    down = gathered(down_weight.T)

    both = jnp.dot(tokens, gate_up, preferred_element_type=jnp.float32)
    gate_pre, up_pre = both[:, :units], both[:, units:]
    sigmoid_gate = jax.nn.sigmoid(gate_pre)
    activated = gate_pre * sigmoid_gate
    hidden = (activated * up_pre).astype(jnp.bfloat16)

    terms = contract_rows(cotangent, hidden).astype(jnp.bfloat16)
    down_grad = scattered(terms, rows).T

    hidden_grad = jnp.dot(cotangent, down, preferred_element_type=jnp.float32)
    gate_pre_grad = (
        hidden_grad * up_pre * sigmoid_gate * (1.0 + gate_pre * (1.0 - sigmoid_gate))
    ).astype(jnp.bfloat16)
    up_pre_grad = (hidden_grad * activated).astype(jnp.bfloat16)
    partial = contract_cols(gate_up, jnp.concatenate([gate_pre_grad, up_pre_grad], axis=1))
    total = summed_over_tp(partial.astype(jnp.bfloat16))
    return (total.T, down_grad)


def solution(mesh):
    torus = Mesh(
        mesh.devices.reshape(FAR, 12 // FAR, 8, mesh.shape["tp"] // 2, 2), (*FS, "chip", "core")
    )
    tp = ("chip", "core")
    in_specs = (P(FS, None), P(FS, None), P(FS, tp), P(FS, tp), P(tp, FS))
    out_specs = (P(FS, None), P(tp, FS))
    return jax.shard_map(
        gradients, mesh=torus, in_specs=in_specs, out_specs=out_specs, check_vma=False
    )
```

```python
import jax
import jax.numpy as jnp
import numpy as np
from jax import lax
from jax.sharding import Mesh
from jax.sharding import PartitionSpec as P


FAR = 4
FS_0 = ("fs_0h", "fs_0l")
FS = (*FS_0, "fs_1")


def shifted(array, axis, step):
    peers = lax.axis_size(axis)
    return lax.ppermute(array, axis, [(k, (k + step) % peers) for k in range(peers)])


def sent_to_all(array, axis):
    peers = lax.axis_size(axis)
    return lax.all_to_all(
        jnp.broadcast_to(array[None], (peers, *array.shape)), axis, 0, 0, tiled=True
    )


def exchanged(parts, axis):
    got = lax.all_to_all(parts, axis, 0, 0, tiled=True)
    return got.astype(jnp.float32).sum(axis=0)


def contract_rows(left, right):
    return lax.dot_general(
        left, right, (((0,), (0,)), ((), ())), preferred_element_type=jnp.float32
    )


def contract_cols(left, right):
    return lax.dot_general(
        left, right, (((1,), (1,)), ((), ())), preferred_element_type=jnp.float32
    )


def picked(source):
    source = jnp.asarray(source, jnp.int32)
    spot = lax.broadcasted_iota(jnp.int32, (source.size, source.size), 1)
    return (source[:, None] == spot).astype(jnp.bfloat16)


def around(block, axis):
    peers = lax.axis_size(axis)
    rows = block.shape[0]
    half = rows // 2
    place = lax.axis_index(axis)

    def put(whole, part, owner, start):
        owner = (owner + peers) % peers
        return lax.dynamic_update_slice(whole, part[None], (owner, start, 0))

    whole = put(jnp.zeros((peers, *block.shape), block.dtype), block, place, 0)
    up = down = block
    for step in range(1, peers // 2):
        up, down = shifted(up, axis, 1), shifted(down, axis, -1)
        whole = put(whole, up, place - step, 0)
        whole = put(whole, down, place + step, 0)
    whole = put(whole, shifted(up[:half], axis, 1), place + peers // 2, 0)
    whole = put(whole, shifted(down[half:], axis, -1), place + peers // 2, half)
    return whole.reshape(peers * rows, -1)


def paired(array, turn):
    chips = lax.axis_size("chip")
    pairs = []
    for chip in range(chips):
        for core in range(2):
            other = (chip + (1 if (chip + core + turn) % 2 == 0 else -1)) % chips
            pairs.append((2 * chip + core, 2 * other + core))
    return lax.ppermute(array, ("chip", "core"), pairs)


def added(left, right):
    return (left.astype(jnp.float32) + right.astype(jnp.float32)).astype(jnp.bfloat16)


def summed_over_tp(partial):
    half = partial.shape[0] // 2
    core = lax.axis_index("core")
    kept = lax.dynamic_slice_in_dim(partial, core * half, half)
    given = lax.dynamic_slice_in_dim(partial, (1 - core) * half, half)
    total = added(kept, shifted(given, "core", 1))
    total = added(total, paired(total, 0))
    other = paired(total, 1)
    total = added(total, other)
    other = shifted(total, "core", 1)
    first = jnp.where(core == 0, total, other)
    second = jnp.where(core == 0, other, total)
    return jnp.concatenate([first, second])


def gradients(tokens, cotangent, gate_weight, up_weight, down_weight):
    near, inner = lax.axis_size("fs_0l"), lax.axis_size("fs_1")
    rows, units = gate_weight.shape
    width = tokens.shape[1]

    gate_up = jnp.concatenate([gate_weight, up_weight], axis=1)
    gate_up = sent_to_all(gate_up, "fs_1").reshape(inner * rows, 2 * units)
    gate_up = around(gate_up, FS_0)
    down = sent_to_all(down_weight.T, FS_0[::-1]).reshape(-1, units)
    down = sent_to_all(down, "fs_1").reshape(width, units)

    spot = np.arange(width).reshape(FAR, near, inner, rows).transpose(2, 1, 0, 3).reshape(-1)
    turned_cotangent = contract_cols(picked(spot), cotangent).astype(jnp.bfloat16)
    turned_cotangent = lax.optimization_barrier(turned_cotangent)

    both = jnp.dot(tokens, gate_up, preferred_element_type=jnp.float32)
    gate_pre, up_pre = both[:, :units], both[:, units:]
    sigmoid_gate = jax.nn.sigmoid(gate_pre)
    activated = gate_pre * sigmoid_gate
    hidden = (activated * up_pre).astype(jnp.bfloat16)

    terms = jnp.dot(turned_cotangent, hidden, preferred_element_type=jnp.float32)
    terms = terms.astype(jnp.bfloat16).reshape(inner * near, FAR * rows, units)
    terms = exchanged(terms, ("fs_1", "fs_0l"))
    terms = terms.astype(jnp.bfloat16).reshape(FAR, rows, units)
    down_grad = exchanged(terms, "fs_0h").T

    hidden_grad = contract_rows(turned_cotangent, down)
    gate_pre_grad = (
        hidden_grad * up_pre * sigmoid_gate * (1.0 + gate_pre * (1.0 - sigmoid_gate))
    ).astype(jnp.bfloat16)
    up_pre_grad = (hidden_grad * activated).astype(jnp.bfloat16)
    partial = contract_cols(gate_up, jnp.concatenate([gate_pre_grad, up_pre_grad], axis=1))
    total = summed_over_tp(partial.astype(jnp.bfloat16))
    return (total.T, down_grad)


def solution(mesh):
    torus = Mesh(
        mesh.devices.reshape(FAR, 12 // FAR, 8, mesh.shape["tp"] // 2, 2), (*FS, "chip", "core")
    )
    tp = ("chip", "core")
    in_specs = (P(FS, None), P(FS, None), P(FS, tp), P(FS, tp), P(tp, FS))
    out_specs = (P(FS, None), P(tp, FS))
    return jax.shard_map(
        gradients, mesh=torus, in_specs=in_specs, out_specs=out_specs, check_vma=False
    )
```

```python
import jax
import jax.numpy as jnp
import numpy as np
from jax import lax
from jax.sharding import Mesh
from jax.sharding import PartitionSpec as P


FAR = 4
FS_0 = ("fs_0h", "fs_0l")
FS = (*FS_0, "fs_1")


def shifted(array, axis, step):
    peers = lax.axis_size(axis)
    return lax.ppermute(array, axis, [(k, (k + step) % peers) for k in range(peers)])


def sent_to_all(array, axis):
    peers = lax.axis_size(axis)
    return lax.all_to_all(
        jnp.broadcast_to(array[None], (peers, *array.shape)), axis, 0, 0, tiled=True
    )


def exchanged(parts, axis):
    got = lax.all_to_all(parts, axis, 0, 0, tiled=True)
    return got.astype(jnp.float32).sum(axis=0)


def contract_cols(left, right):
    return lax.dot_general(
        left, right, (((1,), (1,)), ((), ())), preferred_element_type=jnp.float32
    )


def picked(source):
    source = jnp.asarray(source, jnp.int32)
    spot = lax.broadcasted_iota(jnp.int32, (source.size, source.size), 1)
    return (source[:, None] == spot).astype(jnp.bfloat16)


def around(block, axis, widths):
    peers = lax.axis_size(axis)
    rows = block.shape[0]
    half = rows // 2
    place = lax.axis_index(axis)
    ends = np.cumsum(widths)
    wholes = [jnp.zeros((peers, rows, w), block.dtype) for w in widths]

    def put(part, owner, start):
        owner = (owner + peers) % peers
        for k, (end, w) in enumerate(zip(ends, widths)):
            piece = part[None, :, end - w : end]
            wholes[k] = lax.dynamic_update_slice(wholes[k], piece, (owner, start, 0))

    put(block, place, 0)
    up = down = block
    for step in range(1, peers // 2):
        up, down = shifted(up, axis, 1), shifted(down, axis, -1)
        put(up, place - step, 0)
        put(down, place + step, 0)
    put(shifted(up[:half], axis, 1), place + peers // 2, 0)
    put(shifted(down[half:], axis, -1), place + peers // 2, half)
    return [w.reshape(peers * rows, -1) for w in wholes]


def paired(array, turn):
    chips = lax.axis_size("chip")
    pairs = []
    for chip in range(chips):
        for core in range(2):
            other = (chip + (1 if (chip + core + turn) % 2 == 0 else -1)) % chips
            pairs.append((2 * chip + core, 2 * other + core))
    return lax.ppermute(array, ("chip", "core"), pairs)


def added(left, right):
    return (left.astype(jnp.float32) + right.astype(jnp.float32)).astype(jnp.bfloat16)


def summed_over_tp(partial):
    half = partial.shape[0] // 2
    core = lax.axis_index("core")
    kept = lax.dynamic_slice_in_dim(partial, core * half, half)
    given = lax.dynamic_slice_in_dim(partial, (1 - core) * half, half)
    total = added(kept, shifted(given, "core", 1))
    total = added(total, paired(total, 0))
    other = paired(total, 1)
    total = added(total, other)
    other = shifted(total, "core", 1)
    first = jnp.where(core == 0, total, other)
    second = jnp.where(core == 0, other, total)
    return jnp.concatenate([first, second])


def gradients(tokens, cotangent, gate_weight, up_weight, down_weight):
    near, inner = lax.axis_size("fs_0l"), lax.axis_size("fs_1")
    rows, units = gate_weight.shape
    width = tokens.shape[1]

    weights = jnp.concatenate([gate_weight, up_weight, down_weight.T], axis=1)
    weights = sent_to_all(weights, "fs_1").reshape(inner * rows, 3 * units)
    gate_up, down = around(weights, FS_0, (2 * units, units))

    spot = np.arange(width).reshape(FAR, near, inner, rows).transpose(2, 1, 0, 3).reshape(-1)
    turned_cotangent = contract_cols(picked(spot), cotangent).astype(jnp.bfloat16)
    turned_cotangent = lax.optimization_barrier(turned_cotangent)

    both = jnp.dot(tokens, gate_up, preferred_element_type=jnp.float32)
    gate_pre, up_pre = both[:, :units], both[:, units:]
    sigmoid_gate = jax.nn.sigmoid(gate_pre)
    activated = gate_pre * sigmoid_gate
    hidden = (activated * up_pre).astype(jnp.bfloat16)

    terms = jnp.dot(turned_cotangent, hidden, preferred_element_type=jnp.float32)
    terms = terms.astype(jnp.bfloat16).reshape(inner * near, FAR * rows, units)
    terms = exchanged(terms, ("fs_1", "fs_0l"))
    terms = terms.astype(jnp.bfloat16).reshape(FAR, rows, units)
    down_grad = exchanged(terms, "fs_0h").T

    hidden_grad = jnp.dot(cotangent, down, preferred_element_type=jnp.float32)
    gate_pre_grad = (
        hidden_grad * up_pre * sigmoid_gate * (1.0 + gate_pre * (1.0 - sigmoid_gate))
    ).astype(jnp.bfloat16)
    up_pre_grad = (hidden_grad * activated).astype(jnp.bfloat16)
    partial = contract_cols(gate_up, jnp.concatenate([gate_pre_grad, up_pre_grad], axis=1))
    total = summed_over_tp(partial.astype(jnp.bfloat16))
    return (total.T, down_grad)


def solution(mesh):
    torus = Mesh(
        mesh.devices.reshape(FAR, 12 // FAR, 8, mesh.shape["tp"] // 2, 2), (*FS, "chip", "core")
    )
    tp = ("chip", "core")
    in_specs = (P(FS, None), P(FS, None), P(FS, tp), P(FS, tp), P(tp, FS))
    out_specs = (P(FS, None), P(tp, FS))
    return jax.shard_map(
        gradients, mesh=torus, in_specs=in_specs, out_specs=out_specs, check_vma=False
    )
```

```python
import jax
import jax.numpy as jnp
import numpy as np
from jax import lax
from jax.sharding import Mesh
from jax.sharding import PartitionSpec as P


FAR = 4
FS_0 = ("fs_0h", "fs_0l")
FS = (*FS_0, "fs_1")


def shifted(array, axis, step):
    peers = lax.axis_size(axis)
    return lax.ppermute(array, axis, [(k, (k + step) % peers) for k in range(peers)])


def sent_to_all(array, axis):
    peers = lax.axis_size(axis)
    return lax.all_to_all(
        jnp.broadcast_to(array[None], (peers, *array.shape)), axis, 0, 0, tiled=True
    )


def exchanged(parts, axis):
    got = lax.all_to_all(parts, axis, 0, 0, tiled=True)
    return got.astype(jnp.float32).sum(axis=0)


def contract_rows(left, right):
    return lax.dot_general(
        left, right, (((0,), (0,)), ((), ())), preferred_element_type=jnp.float32
    )


def contract_cols(left, right):
    return lax.dot_general(
        left, right, (((1,), (1,)), ((), ())), preferred_element_type=jnp.float32
    )


def picked(source):
    source = jnp.asarray(source, jnp.int32)
    spot = lax.broadcasted_iota(jnp.int32, (source.size, source.size), 1)
    return (source[:, None] == spot).astype(jnp.bfloat16)


def around(block, axis, widths):
    peers = lax.axis_size(axis)
    rows = block.shape[0]
    half = rows // 16 * 8
    place = lax.axis_index(axis)
    ends = np.cumsum(widths)
    wholes = [jnp.zeros((peers, rows, w), block.dtype) for w in widths]

    def put(part, owner, start):
        owner = (owner + peers) % peers
        for k, (end, w) in enumerate(zip(ends, widths)):
            piece = part[None, :, end - w : end]
            wholes[k] = lax.dynamic_update_slice(wholes[k], piece, (owner, start, 0))

    put(block, place, 0)
    up = down = block
    for step in range(1, peers // 2):
        up, down = shifted(up, axis, 1), shifted(down, axis, -1)
        put(up, place - step, 0)
        put(down, place + step, 0)
    put(shifted(up[:half], axis, 1), place + peers // 2, 0)
    put(shifted(down[half:], axis, -1), place + peers // 2, half)
    return [w.reshape(peers * rows, -1) for w in wholes]


def paired(array, turn):
    chips = lax.axis_size("chip")
    pairs = []
    for chip in range(chips):
        for core in range(2):
            other = (chip + (1 if (chip + core + turn) % 2 == 0 else -1)) % chips
            pairs.append((2 * chip + core, 2 * other + core))
    return lax.ppermute(array, ("chip", "core"), pairs)


def added(left, right):
    return (left.astype(jnp.float32) + right.astype(jnp.float32)).astype(jnp.bfloat16)


def summed_over_tp(partial, back, blocks):
    half = partial.shape[0] // 2
    core = lax.axis_index("core")
    kept = lax.dynamic_slice_in_dim(partial, core * half, half)
    given = lax.dynamic_slice_in_dim(partial, (1 - core) * half, half)
    total = added(kept, shifted(given, "core", 1))
    total = jnp.dot(back, total, preferred_element_type=jnp.float32).astype(jnp.bfloat16)
    total = added(total, paired(total, 0))
    other = paired(total, 1)
    total = added(total, other)
    other = shifted(total, "core", 1)
    first = jnp.where(core == 0, total, other)
    second = jnp.where(core == 0, other, total)
    halves = [h.reshape(blocks, -1, h.shape[1]) for h in (first, second)]
    return jnp.stack(halves, axis=1).reshape(partial.shape)


def gradients(tokens, cotangent, gate_weight, up_weight, down_weight):
    near, inner = lax.axis_size("fs_0l"), lax.axis_size("fs_1")
    rows, units = gate_weight.shape
    width = tokens.shape[1]

    weights = jnp.concatenate([gate_weight, up_weight, down_weight.T], axis=1)
    weights = sent_to_all(weights, FS_0[::-1]).reshape(-1, 3 * units)
    gate_up, down = around(weights, ("fs_1",), (2 * units, units))

    spot = np.arange(width).reshape(FAR, near, inner, rows).transpose(2, 1, 0, 3).reshape(-1)
    turn = lax.optimization_barrier(picked(spot))
    turned_tokens = contract_cols(turn, tokens).astype(jnp.bfloat16)
    turned_cotangent = contract_cols(turn, cotangent).astype(jnp.bfloat16)
    back = np.arange(width // 2).reshape(-1, near, FAR, rows).transpose(2, 1, 0, 3).reshape(-1)
    turned_tokens, turned_cotangent, back = lax.optimization_barrier(
        (turned_tokens, turned_cotangent, picked(back))
    )

    both = contract_rows(turned_tokens, gate_up)
    gate_pre, up_pre = both[:, :units], both[:, units:]
    sigmoid_gate = jax.nn.sigmoid(gate_pre)
    activated = gate_pre * sigmoid_gate
    hidden = (activated * up_pre).astype(jnp.bfloat16)

    terms = jnp.dot(turned_cotangent, hidden, preferred_element_type=jnp.float32)
    terms = terms.astype(jnp.bfloat16).reshape(inner * near, FAR * rows, units)
    terms = exchanged(terms, ("fs_1", "fs_0l"))
    terms = terms.astype(jnp.bfloat16).reshape(FAR, rows, units)
    down_grad = exchanged(terms, "fs_0h").T

    hidden_grad = contract_rows(turned_cotangent, down)
    gate_pre_grad = (
        hidden_grad * up_pre * sigmoid_gate * (1.0 + gate_pre * (1.0 - sigmoid_gate))
    ).astype(jnp.bfloat16)
    up_pre_grad = (hidden_grad * activated).astype(jnp.bfloat16)
    partial = contract_cols(gate_up, jnp.concatenate([gate_pre_grad, up_pre_grad], axis=1))
    total = summed_over_tp(partial.astype(jnp.bfloat16), back, near * FAR)
    return (total.T, down_grad)


def solution(mesh):
    torus = Mesh(
        mesh.devices.reshape(FAR, 12 // FAR, 8, mesh.shape["tp"] // 2, 2), (*FS, "chip", "core")
    )
    tp = ("chip", "core")
    in_specs = (P(FS, None), P(FS, None), P(FS, tp), P(FS, tp), P(tp, FS))
    out_specs = (P(FS, None), P(tp, FS))
    return jax.shard_map(
        gradients, mesh=torus, in_specs=in_specs, out_specs=out_specs, check_vma=False
    )
```

```python
import jax
import jax.numpy as jnp
import numpy as np
from jax import lax
from jax.sharding import Mesh
from jax.sharding import PartitionSpec as P


FAR = 4
FS_0 = ("fs_0h", "fs_0l")
FS = (*FS_0, "fs_1")


def shifted(array, axis, step):
    peers = lax.axis_size(axis)
    return lax.ppermute(array, axis, [(k, (k + step) % peers) for k in range(peers)])


def sent_to_all(array, axis):
    peers = lax.axis_size(axis)
    return lax.all_to_all(
        jnp.broadcast_to(array[None], (peers, *array.shape)), axis, 0, 0, tiled=True
    )


def exchanged(parts, axis):
    got = lax.all_to_all(parts, axis, 0, 0, tiled=True)
    return got.astype(jnp.float32).sum(axis=0)


def contract_rows(left, right):
    return lax.dot_general(
        left, right, (((0,), (0,)), ((), ())), preferred_element_type=jnp.float32
    )


def contract_cols(left, right):
    return lax.dot_general(
        left, right, (((1,), (1,)), ((), ())), preferred_element_type=jnp.float32
    )


def picked(source):
    source = jnp.asarray(source, jnp.int32)
    spot = lax.broadcasted_iota(jnp.int32, (source.size, source.size), 1)
    return (source[:, None] == spot).astype(jnp.bfloat16)


def around(block, axis, widths):
    peers = lax.axis_size(axis)
    rows = block.shape[0]
    place = lax.axis_index(axis)
    ends = np.cumsum(widths)
    wholes = [jnp.zeros((peers, rows, w), block.dtype) for w in widths]

    def put(part, owner, start):
        owner = (owner + peers) % peers
        for k, (end, w) in enumerate(zip(ends, widths)):
            piece = part[None, :, end - w : end]
            wholes[k] = lax.dynamic_update_slice(wholes[k], piece, (owner, start, 0))

    put(block, place, 0)
    up = down = block
    for step in range(1, peers // 2):
        up, down = shifted(up, axis, 1), shifted(down, axis, -1)
        put(up, place - step, 0)
        put(down, place + step, 0)
    last = jnp.where(lax.axis_index("core") == 0, up, down)
    pairs = [
        (2 * k + core, 2 * ((k + 1 - 2 * core) % peers) + core)
        for k in range(peers)
        for core in range(2)
    ]
    put(lax.ppermute(last, (*axis, "core"), pairs), place + peers // 2, 0)
    return [w.reshape(peers * rows, -1) for w in wholes]


def paired(array, turn):
    chips = lax.axis_size("chip")
    pairs = []
    for chip in range(chips):
        for core in range(2):
            other = (chip + (1 if (chip + core + turn) % 2 == 0 else -1)) % chips
            pairs.append((2 * chip + core, 2 * other + core))
    return lax.ppermute(array, ("chip", "core"), pairs)


def added(left, right):
    return (left.astype(jnp.float32) + right.astype(jnp.float32)).astype(jnp.bfloat16)


def summed_over_tp(partial, back, blocks):
    half = partial.shape[0] // 2
    core = lax.axis_index("core")
    kept = lax.dynamic_slice_in_dim(partial, core * half, half)
    given = lax.dynamic_slice_in_dim(partial, (1 - core) * half, half)
    total = added(kept, shifted(given, "core", 1))
    total = jnp.dot(back, total, preferred_element_type=jnp.float32).astype(jnp.bfloat16)
    total = added(total, paired(total, 0))
    other = paired(total, 1)
    total = added(total, other)
    other = shifted(total, "core", 1)
    first = jnp.where(core == 0, total, other)
    second = jnp.where(core == 0, other, total)
    halves = [h.reshape(blocks, -1, h.shape[1]) for h in (first, second)]
    return jnp.stack(halves, axis=1).reshape(partial.shape)


def gradients(tokens, cotangent, gate_weight, up_weight, down_weight):
    near, inner = lax.axis_size("fs_0l"), lax.axis_size("fs_1")
    rows, units = gate_weight.shape
    width = tokens.shape[1]

    weights = jnp.concatenate([gate_weight, up_weight, down_weight.T], axis=1)
    weights = sent_to_all(weights, FS_0[::-1]).reshape(-1, 3 * units)
    gate_up, down = around(weights, ("fs_1",), (2 * units, units))

    spot = np.arange(width).reshape(FAR, near, inner, rows).transpose(2, 1, 0, 3).reshape(-1)
    turn = lax.optimization_barrier(picked(spot))
    turned_tokens = contract_cols(turn, tokens).astype(jnp.bfloat16)
    turned_cotangent = contract_cols(turn, cotangent).astype(jnp.bfloat16)
    back = np.arange(width // 2).reshape(-1, near, FAR, rows).transpose(2, 1, 0, 3).reshape(-1)
    turned_tokens, turned_cotangent, back = lax.optimization_barrier(
        (turned_tokens, turned_cotangent, picked(back))
    )

    both = contract_rows(turned_tokens, gate_up)
    gate_pre, up_pre = both[:, :units], both[:, units:]
    sigmoid_gate = jax.nn.sigmoid(gate_pre)
    activated = gate_pre * sigmoid_gate
    hidden = (activated * up_pre).astype(jnp.bfloat16)

    terms = jnp.dot(turned_cotangent, hidden, preferred_element_type=jnp.float32)
    terms = terms.astype(jnp.bfloat16).reshape(inner * near, FAR * rows, units)
    terms = exchanged(terms, ("fs_1", "fs_0l"))
    terms = terms.astype(jnp.bfloat16).reshape(FAR, rows, units)
    down_grad = exchanged(terms, "fs_0h").T

    hidden_grad = contract_rows(turned_cotangent, down)
    gate_pre_grad = (
        hidden_grad * up_pre * sigmoid_gate * (1.0 + gate_pre * (1.0 - sigmoid_gate))
    ).astype(jnp.bfloat16)
    up_pre_grad = (hidden_grad * activated).astype(jnp.bfloat16)
    partial = contract_cols(gate_up, jnp.concatenate([gate_pre_grad, up_pre_grad], axis=1))
    total = summed_over_tp(partial.astype(jnp.bfloat16), back, near * FAR)
    return (total.T, down_grad)


def solution(mesh):
    torus = Mesh(
        mesh.devices.reshape(FAR, 12 // FAR, 8, mesh.shape["tp"] // 2, 2), (*FS, "chip", "core")
    )
    tp = ("chip", "core")
    in_specs = (P(FS, None), P(FS, None), P(FS, tp), P(FS, tp), P(tp, FS))
    out_specs = (P(FS, None), P(tp, FS))
    return jax.shard_map(
        gradients, mesh=torus, in_specs=in_specs, out_specs=out_specs, check_vma=False
    )
```
